32 devices in a mesh: ep: 16 (over z, y, x), tp: 2 (over core).
Axes of the slice: x: 2, y: 2, z: 4, core: 2. Of those that a mesh axis runs over, the one named last changes fastest.
Arguments:
- tokens: bfloat16 [256, 1536], P('ep'), may hold values from -6 to 6
- prior_state: float32 [256, 12, 64, 64], P('ep', 'tp'), may hold values from -12 to 12
- first_gain: float32 [1536], replicated, may hold values from 0.1 to 1.9
- query_weight: bfloat16 [1536, 768], P(None, 'tp'), may hold values from -0.15625 to 0.15625
- key_weight: bfloat16 [1536, 768], P(None, 'tp'), may hold values from -0.15625 to 0.15625
- value_weight: bfloat16 [1536, 768], P(None, 'tp'), may hold values from -0.15625 to 0.15625
- decay_down: bfloat16 [1536, 96], replicated, may hold values from -0.15625 to 0.15625
- decay_up: bfloat16 [96, 768], P(None, 'tp'), may hold values from -1.25 to 1.25
- decay_base: float32 [768], P('tp'), may hold values from -5 to 1
- rate_down: bfloat16 [1536, 96], replicated, may hold values from -0.15625 to 0.15625
- rate_up: bfloat16 [96, 768], P(None, 'tp'), may hold values from -1.25 to 1.25
- rate_base: float32 [768], P('tp'), may hold values from -4 to 4
- head_gain: float32 [768], P('tp'), may hold values from 0.1 to 1.9
- out_weight: bfloat16 [768, 1536], P('tp'), may hold values from -0.21875 to 0.21875
- mid_gain: float32 [1536], replicated, may hold values from 0.1 to 1.9
- route_ids: int32 [256, 6], P('ep'), may hold values from 0 to 15, all different within a row; in each aligned block of 16 rows (0 to 15, 16 to 31, ...) at most 12 rows name the same one
- route_weights: float32 [256, 6], P('ep'), may hold values from 0.1 to 1
- expert_gate: bfloat16 [16, 1536, 384], P('ep', None, 'tp'), may hold values from -0.15625 to 0.15625
- expert_up: bfloat16 [16, 1536, 384], P('ep', None, 'tp'), may hold values from -0.15625 to 0.15625
- expert_down: bfloat16 [16, 384, 1536], P('ep', 'tp'), may hold values from -0.3125 to 0.3125
- dense_gate: bfloat16 [1536, 6144], P(None, ('ep', 'tp')), may hold values from -0.15625 to 0.15625
- dense_up: bfloat16 [1536, 6144], P(None, ('ep', 'tp')), may hold values from -0.15625 to 0.15625
- dense_down: bfloat16 [6144, 1536], P(('ep', 'tp')), may hold values from -0.078125 to 0.078125
- blend_vector: bfloat16 [1536], replicated, may hold values from -0.15625 to 0.15625
Outputs:
- mixed: bfloat16 [256, 1536], P('ep', 'tp')
- new_state: float32 [256, 12, 64, 64], P('ep', 'tp')
The draws below stay inside these ranges and needn't reach their ends.
Inputs may be any that keep to these rules, and one draw needn't show every extreme that they name: `route_ids`: each row names 6 different experts; among the rows of one device no expert is named by more than 12 rows, a bound that some block reaches.
All inputs are finite; a program needn't handle non-finite values.
Results may differ from the reference program's by a relative error of at most 0.02.
Values may be sent and summed in bfloat16 or wider, within the bound.
A program may use at most 128 MiB of HBM per device.

```python
import math
import jax
import jax.numpy as jnp
import numpy as np
from jax import lax

D = 1536
HEADS = 12
HEAD = 64
INNER = 768
RANK = 96
FE = 384
FD = 6144
TOP = 6
SEQS = 16
EXPERTS = 16
BATCH = 256
CAP = 12
N_EP = 16
N_TP = 2


def levels(key, extent, pieces, least, largest):
    level = 1.0
    for axis_at, parts in pieces:
        draws = jax.random.uniform(jax.random.fold_in(jax.random.fold_in(key, 6), axis_at), (parts,), jnp.float32, least / len(pieces), largest / len(pieces))
        level = level * jnp.repeat(jnp.exp(draws), extent[axis_at] // parts).reshape((-1,) + (1,) * (len(extent) - 1 - axis_at))
    return level


def shared_out(rng, own, number, rows, count, top, bound, slope):
    sequence = jax.random.permutation(rng, count)
    crowded, common = shares(count, rows * top, bound, slope, True), shares(count, rows * top, bound, slope, False)
    places = jnp.arange(count)

    def named(tallies, offset_by):
        used = int((tallies > 0).sum())
        fixed = max(1, used // 4)
        passed = fixed + (places - fixed + offset_by * (used - fixed)) % max(1, count - fixed)
        return jnp.zeros((count,), jnp.int32).at[sequence[jnp.where(places < fixed, places, passed)]].set(jnp.asarray(tallies, jnp.int32))

    tallies = jnp.where(number % 4 == 0, named(crowded, number // 4), named(common, number - number // 4 - 1))
    mixed = jax.random.permutation(jax.random.fold_in(own, 3), count)
    donor, taker = mixed[0:count // 2 * 2:2], mixed[1:count // 2 * 2:2]
    room = jnp.minimum(tallies[donor] - 1, bound - tallies[taker]) // 2
    room = jnp.where((donor == sequence[0]) | (taker == sequence[0]) | (tallies[taker] == 0), 0, jnp.maximum(room, 0))
    passed = jax.random.randint(jax.random.fold_in(own, 4), (count // 2,), 0, 1 << 20) % (room + 1)
    tallies = tallies.at[donor].add(-passed).at[taker].add(passed)
    items = jnp.searchsorted(jnp.cumsum(tallies), jnp.arange(rows * top), side="right").astype(jnp.int32)
    table = items.reshape(top, rows).T
    table = table[jax.random.permutation(jax.random.fold_in(own, 1), rows)]
    offset_by = jax.random.randint(jax.random.fold_in(own, 2), (rows, 1), 0, top)
    return jnp.take_along_axis(table, (jnp.arange(top)[None, :] + offset_by) % top, axis=1)


def shares(amount, total, limit, skew, full):
    portions = [(1 << 20) // math.isqrt(standing ** skew) + 1 for standing in range(1, amount + 1)]
    largest = limit if full else min(limit, max(-(-total // amount), total * portions[0] // sum(portions)))
    least = 1 if total - largest >= amount - 1 else 0
    holding, spare = [largest] + [least] * (amount - 1), total - largest - least * (amount - 1)
    while spare > 0:
        free = [i for i in range(1, amount) if holding[i] < largest] or [i for i in range(1, amount) if holding[i] < limit]
        whole, left = sum([portions[i] for i in free]), spare
        for i in free:
            extra = min(limit - holding[i], max(1, left * portions[i] // whole), spare)
            holding[i] = holding[i] + extra
            spare = spare - extra
    return np.array(holding)


def gaussian(stream_key, shape, width, limit, split=(), kind=jnp.bfloat16):
    result = jax.random.normal(stream_key, shape, jnp.float32) * width
    if len(split) > 0:
        result = levels(stream_key, shape, split, -0.22, 0.18) * result
    return jnp.clip(result, min=-limit, max=limit).astype(kind)


def setup_inputs(seed: int = 0) -> dict:
    key_list = jax.random.split(jax.random.key(seed), 25)
    tokens = gaussian(key_list[0], (BATCH, D), 1.0, 6.0, ((0, 16),))
    prior_state = gaussian(key_list[1], (BATCH, HEADS, HEAD, HEAD), 2.0, 12.0, ((0, 16), (1, 2)), jnp.float32)
    first_gain = jnp.clip(1.0 + 0.18 * jax.random.normal(key_list[2], (D,), jnp.float32), 0.1, 1.9)
    query_weight = gaussian(key_list[3], (D, INNER), D ** -0.5, 0.15625, ((1, 2),))
    key_weight = gaussian(key_list[4], (D, INNER), D ** -0.5, 0.15625, ((1, 2),))
    value_weight = gaussian(key_list[5], (D, INNER), D ** -0.5, 0.15625, ((1, 2),))
    decay_down = gaussian(key_list[6], (D, RANK), D ** -0.5, 0.15625)
    decay_up = gaussian(key_list[7], (RANK, INNER), (RANK // 4) ** -0.5, 1.25, ((1, 2),))
    decay_base = jnp.clip(-5.0 + 6.0 * jax.random.uniform(key_list[8], (INNER,), jnp.float32) ** levels(key_list[8], (INNER,), ((0, 2),), -0.2, 0.2), -5.0, 1.0)
    rate_down = gaussian(key_list[9], (D, RANK), D ** -0.5, 0.15625)
    rate_up = gaussian(key_list[10], (RANK, INNER), (RANK // 4) ** -0.5, 1.25, ((1, 2),))
    rate_base = jnp.clip(jax.random.uniform(key_list[11], (INNER,), jnp.float32, -4.0, 4.0) * levels(key_list[11], (INNER,), ((0, 2),), -0.4, 0.0), -4.0, 4.0)
    head_gain = jnp.clip(1.0 + 0.18 * jax.random.normal(key_list[12], (INNER,), jnp.float32), 0.1, 1.9)
    out_weight = gaussian(key_list[13], (INNER, D), INNER ** -0.5, 0.21875, ((0, 2),))
    mid_gain = jnp.clip(1.0 + 0.18 * jax.random.normal(key_list[14], (D,), jnp.float32), 0.1, 1.9)
    route_ids_keys = jax.random.split(jax.random.fold_in(key_list[15], 1), BATCH // SEQS)
    route_ids_turns = jax.random.permutation(jax.random.fold_in(key_list[15], 3), BATCH // SEQS)
    route_ids = jax.vmap(lambda own, number: shared_out(jax.random.fold_in(key_list[15], 2), own, number, SEQS, EXPERTS, TOP, CAP, 2))(route_ids_keys, route_ids_turns).reshape((BATCH, TOP))
    route_weights = jnp.clip(jnp.exp(math.log(1.0) - 2.3025851 * jax.random.uniform(key_list[16], (BATCH, TOP), jnp.float32) ** levels(key_list[16], (BATCH, TOP), ((0, 16),), -0.2, 0.2)), 0.1, 1.0)
    expert_gate = gaussian(key_list[17], (EXPERTS, D, FE), D ** -0.5, 0.15625, ((0, 16), (2, 2)))
    expert_up = gaussian(key_list[18], (EXPERTS, D, FE), D ** -0.5, 0.15625, ((0, 16), (2, 2)))
    expert_down = gaussian(key_list[19], (EXPERTS, FE, D), FE ** -0.5, 0.3125, ((0, 16), (1, 2)))
    dense_gate = gaussian(key_list[20], (D, FD), D ** -0.5, 0.15625, ((1, 32),))
    dense_up = gaussian(key_list[21], (D, FD), D ** -0.5, 0.15625, ((1, 32),))
    dense_down = gaussian(key_list[22], (FD, D), FD ** -0.5, 0.078125, ((0, 32),))
    blend_vector = gaussian(key_list[23], (D,), D ** -0.5, 0.15625)
    return dict(tokens=tokens, prior_state=prior_state, first_gain=first_gain, query_weight=query_weight, key_weight=key_weight, value_weight=value_weight, decay_down=decay_down, decay_up=decay_up, decay_base=decay_base, rate_down=rate_down, rate_up=rate_up, rate_base=rate_base, head_gain=head_gain, out_weight=out_weight, mid_gain=mid_gain, route_ids=route_ids, route_weights=route_weights, expert_gate=expert_gate, expert_up=expert_up, expert_down=expert_down, dense_gate=dense_gate, dense_up=dense_up, dense_down=dense_down, blend_vector=blend_vector)


def rms_norm(values, gain):
    scale = lax.rsqrt(lax.optimization_barrier(jnp.mean(values * values, axis=-1, keepdims=True)) + 1e-06)
    return values * scale * gain.astype(jnp.float32)

def rounded(values):
    return lax.optimization_barrier(values.astype(jnp.bfloat16)).astype(jnp.float32)

def mixer_core(normed, prior_state, query_weight, key_weight, value_weight, decay_down, decay_up, decay_base, rate_down, rate_up, rate_base, head_gain):
    rows = normed.shape[0]
    heads_here = prior_state.shape[1]
    head_size = prior_state.shape[2]

    def project(weight):
        product = jnp.dot(normed, weight, preferred_element_type=jnp.float32)
        return rounded(product).reshape(rows, heads_here, head_size)
    receptance = project(query_weight)
    key_vec = project(key_weight)
    value_vec = project(value_weight)
    decay_low = jnp.tanh(jnp.dot(normed, decay_down, preferred_element_type=jnp.float32)).astype(jnp.bfloat16)
    decay_log = decay_base + jnp.dot(decay_low, decay_up, preferred_element_type=jnp.float32)
    decay_log = -jax.nn.softplus(-decay_log) - 0.5
    decay_rate = jnp.exp(-jnp.exp(decay_log)).reshape(rows, heads_here, head_size)
    rate_low = jnp.dot(normed, rate_down, preferred_element_type=jnp.float32).astype(jnp.bfloat16)
    learn_rate = jax.nn.sigmoid(rate_base + jnp.dot(rate_low, rate_up, preferred_element_type=jnp.float32))
    learn_rate = learn_rate.reshape(rows, heads_here, head_size)
    unit_key = key_vec * lax.rsqrt(lax.optimization_barrier(jnp.sum(key_vec * key_vec, axis=-1, keepdims=True)) + 1e-06)
    removed = lax.optimization_barrier(jnp.sum(prior_state * unit_key[:, :, None, :], axis=-1))
    new_state = prior_state * decay_rate[:, :, None, :] - removed[..., None] * (unit_key * learn_rate)[:, :, None, :] + value_vec[..., None] * key_vec[:, :, None, :]
    read = lax.optimization_barrier(jnp.sum(new_state * receptance[:, :, None, :], axis=-1))
    center = lax.optimization_barrier(jnp.mean(read, axis=-1, keepdims=True))
    spread = lax.optimization_barrier(jnp.mean(jnp.square(read - center), axis=-1, keepdims=True))
    normal = (read - center) * lax.rsqrt(spread + 0.00064)
    mixed_heads = (normal.reshape(rows, -1) * head_gain.astype(jnp.float32)).astype(jnp.bfloat16)
    return (mixed_heads, new_state)

def reference(tokens, prior_state, first_gain, query_weight, key_weight, value_weight, decay_down, decay_up, decay_base, rate_down, rate_up, rate_base, head_gain, out_weight, mid_gain, route_ids, route_weights, expert_gate, expert_up, expert_down, dense_gate, dense_up, dense_down, blend_vector):
    token_f = tokens.astype(jnp.float32)
    normed = rms_norm(token_f, first_gain).astype(jnp.bfloat16)
    mixed_heads, new_state = mixer_core(normed, prior_state, query_weight, key_weight, value_weight, decay_down, decay_up, decay_base, rate_down, rate_up, rate_base, head_gain)
    block = INNER // N_TP
    attn = jnp.zeros((BATCH, D), jnp.float32)
    for part_idx in range(N_TP):
        lower = part_idx * block
        attn = attn + rounded(jnp.dot(mixed_heads[:, lower:lower + block], out_weight[lower:lower + block], preferred_element_type=jnp.float32))
    resid = rounded(token_f + attn)
    mid = rms_norm(resid, mid_gain).astype(jnp.bfloat16)
    blend = jax.nn.sigmoid(jnp.dot(mid, blend_vector, preferred_element_type=jnp.float32))
    flat_ids = route_ids.reshape(N_EP, SEQS * TOP)
    onehot = (flat_ids[..., None] == jnp.arange(EXPERTS, dtype=jnp.int32)[None, None, :]).astype(jnp.int32)
    before = jnp.cumsum(onehot, axis=1) - onehot
    position = lax.optimization_barrier(jnp.sum(onehot * before, axis=-1))
    group_ids = jnp.arange(N_EP, dtype=jnp.int32)[:, None]
    slot = (flat_ids * (N_EP * CAP) + group_ids * CAP + position).reshape(-1).astype(jnp.int32)
    sources = jnp.repeat(mid, TOP, axis=0)
    buffer = jnp.zeros((EXPERTS * N_EP * CAP, D), jnp.bfloat16).at[slot].set(sources)
    buffer = buffer.reshape(EXPERTS, N_EP * CAP, D)
    half_units = FE // N_TP

    def run_expert(items):
        rows_in, gate_w, up_w, down_w = items
        hidden = (jax.nn.silu(jnp.dot(rows_in, gate_w, preferred_element_type=jnp.float32)) * jnp.dot(rows_in, up_w, preferred_element_type=jnp.float32)).astype(jnp.bfloat16)
        total = jnp.zeros((rows_in.shape[0], D), jnp.float32)
        for part_idx in range(N_TP):
            lower = part_idx * half_units
            total = total + rounded(jnp.dot(hidden[:, lower:lower + half_units], down_w[lower:lower + half_units], preferred_element_type=jnp.float32))
        return total.astype(jnp.bfloat16)
    outputs = lax.map(run_expert, (buffer, expert_gate, expert_up, expert_down)).reshape(-1, D)
    picked = outputs[slot].astype(jnp.float32).reshape(BATCH, TOP, D)
    share = route_weights / lax.optimization_barrier(jnp.sum(route_weights, axis=1, keepdims=True)) * 2.5
    routed = lax.optimization_barrier(jnp.sum(share[..., None] * picked, axis=1))
    dense_hidden = (jax.nn.silu(jnp.dot(mid, dense_gate, preferred_element_type=jnp.float32)) * jnp.dot(mid, dense_up, preferred_element_type=jnp.float32)).astype(jnp.bfloat16)
    dense_out = jnp.dot(dense_hidden, dense_down, preferred_element_type=jnp.float32)
    mixed = (resid + routed + blend[:, None] * dense_out).astype(jnp.bfloat16)
    return (mixed, new_state)
```

```python
import functools

import jax
import jax.numpy as jnp
from jax import lax
from jax.experimental import pallas as pl
from jax.experimental.pallas import tpu as pltpu
from jax.sharding import PartitionSpec as P

MESH = pl.DeviceIdType.MESH
F32 = jnp.float32
BF16 = jnp.bfloat16
ANY = pl.BlockSpec(memory_space=pl.ANY)
VMEM = pl.BlockSpec(memory_space=pltpu.VMEM)


def dot(a, b):
    return jnp.dot(a, b, preferred_element_type=F32)


def dot_t(a, b):
    return lax.dot_general(a, b, (((1,), (1,)), ((), ())), preferred_element_type=F32)


def sigmoid(x):
    return 1.0 / (1.0 + jnp.exp(-x))


def front_kernel(
    tok, state, gain, wq, wk, wv, dd, du, db, rd, ru, rb, hg, ow,
    part, new_state,
    q_v, k_v, v_v, ow_v, st, sto, vec, reads, wsem, isem, osem,
):
    rows, heads, size = st.shape[0], st.shape[1], st.shape[2]
    weights = [
        pltpu.make_async_copy(src, dst, wsem.at[i])
        for i, (src, dst) in enumerate(((wk, k_v), (wq, q_v), (wv, v_v), (ow, ow_v)))
    ]
    for copy in weights[:3]:
        copy.start()

    def state_in(r):
        return pltpu.make_async_copy(state.at[r], st.at[r], isem.at[r])

    def state_out(r):
        return pltpu.make_async_copy(sto.at[r], new_state.at[r], osem.at[r])

    for r in range(rows):
        state_in(r).start()
    weights[3].start()

    x = tok[...].astype(F32)
    scale = lax.rsqrt(jnp.mean(x * x, axis=-1, keepdims=True) + 1e-06)
    normed = (x * scale * gain[...][None, :]).astype(BF16)
    low = jnp.tanh(dot_t(normed, dd[...])).astype(BF16)
    decay = jnp.exp(-0.6065306597126334 * sigmoid(db[...][None, :] + dot(low, du[...])))
    rlow = dot_t(normed, rd[...]).astype(BF16)
    rate = sigmoid(rb[...][None, :] + dot(rlow, ru[...]))
    weights[0].wait()
    key = dot(normed, k_v[...]).astype(BF16).astype(F32)
    weights[1].wait()
    rec = dot(normed, q_v[...]).astype(BF16).astype(F32)
    weights[2].wait()
    val = dot(normed, v_v[...]).astype(BF16).astype(F32)
    for h in range(heads):
        at = slice(h * size, (h + 1) * size)
        kh = key[:, at]
        unit = kh * lax.rsqrt(jnp.sum(kh * kh, axis=-1, keepdims=True) + 1e-06)
        vec[0, h] = unit
        vec[1, h] = decay[:, at]
        vec[2, h] = unit * rate[:, at]
        vec[3, h] = kh
        vec[4, h] = rec[:, at]
        vec[5, h] = val[:, at]

    eye = lax.broadcasted_iota(jnp.int32, (size, size), 0) == lax.broadcasted_iota(
        jnp.int32, (size, size), 1
    )

    def step(r, carry):
        state_in(r).wait()
        for h in range(heads):
            unit, dec, ul, kh, qh, vh = [vec[j, h, pl.ds(r, 1), :] for j in range(6)]
            s = st[r, h]
            removed = jnp.sum(s * unit, axis=-1, keepdims=True)
            vcol = jnp.sum(jnp.where(eye, vh, 0.0), axis=-1, keepdims=True)
            new = s * dec - removed * ul + vcol * kh
            sto[r, h] = new
            read = jnp.sum(new * qh, axis=-1, keepdims=True)
            reads[h, pl.ds(r, 1), :] = jnp.sum(jnp.where(eye, read, 0.0), axis=0, keepdims=True)
        state_out(r).start()
        return carry

    lax.fori_loop(0, rows, step, 0)
    weights[3].wait()
    total = None
    for h in range(heads):
        at = slice(h * size, (h + 1) * size)
        read = reads[h]
        read = read - jnp.mean(read, axis=-1, keepdims=True)
        spread = jnp.mean(read * read, axis=-1, keepdims=True)
        mixed = (read * lax.rsqrt(spread + 0.00064) * hg[...][None, :][:, at]).astype(BF16)
        term = dot(mixed, ow_v[h * size : (h + 1) * size, :])
        total = term if total is None else total + term
    part[...] = total.astype(BF16)

    def drain(r, carry):
        state_out(r).wait()
        return carry

    lax.fori_loop(0, rows, drain, 0)


def back_kernel(
    count, plane,
    tok, part, gain, ids, scores, blend_vec, eg, eu, ed, dg, du, dn,
    out,
    eg_v, eu_v, ed_v, dg_v, du_v, dn_v, prx, gbuf, res, hid_e, hid_d, own, ds2, dr2, r1s, r1r, r2s, r2r,
    wsem, xs, xr, agr, zs, ps, fs, fr, d2s, d2r, s1, r1, s2, r2,
):
    e = lax.axis_index("ep")
    t = lax.axis_index("tp")
    other = 1 - t
    depth = count // plane
    z, p = e // plane, e % plane
    seqs, width = tok.shape
    half = width // 2
    tail = gbuf.shape[3] - half
    top = ids.shape[0]

    barrier = pltpu.get_barrier_semaphore()

    def greet(device):
        pl.semaphore_signal(barrier, inc=1, device_id=device, device_id_type=MESH)

    def at_z(dz):
        return (z + dz) % depth

    def at_p(dp):
        return (p + dp) % plane

    greet((e, other))
    for dz in range(1, depth):
        greet((at_z(dz) * plane + p, t))
    for dp in range(1, plane):
        greet((z * plane + at_p(dp), t))

    weights = [
        pltpu.make_async_copy(src, dst, wsem.at[i])
        for i, (src, dst) in enumerate(
            ((eg.at[0], eg_v), (eu.at[0], eu_v), (dg, dg_v), (du, du_v), (ed.at[0], ed_v), (dn, dn_v))
        )
    ]
    for copy in weights:
        copy.start()

    def remote(src, dst, send, recv, device):
        return pltpu.make_async_remote_copy(
            src_ref=src, dst_ref=dst, send_sem=send, recv_sem=recv,
            device_id=device, device_id_type=MESH,
        )

    lanes = lax.broadcasted_iota(jnp.int32, (seqs, tail), 1)
    score = scores[...]
    share = score / jnp.sum(score, axis=0, keepdims=True) * 2.5
    id_all = ids[...].astype(F32)
    eye = lax.broadcasted_iota(jnp.int32, (seqs, seqs), 0) == lax.broadcasted_iota(
        jnp.int32, (seqs, seqs), 1
    )

    def column(row):
        return jnp.sum(jnp.where(eye, row, 0.0), axis=1, keepdims=True)

    table = jnp.zeros((seqs, tail), F32)
    for k in range(top):
        named = lanes.astype(F32) == column(id_all[k : k + 1, :])
        table = table + jnp.where(named, column(share[k : k + 1, :]), 0.0)

    pl.semaphore_wait(barrier, 1 + (depth - 1) + (plane - 1))
    swap = remote(part, prx, xs, xr, (e, other))
    swap.start()
    token_f = tok[...].astype(F32)
    swap.wait()
    resid = (token_f + (part[...].astype(F32) + prx[...].astype(F32))).astype(BF16).astype(F32)
    res[0] = resid[:, :half]
    res[1] = resid[:, half:]
    scale = lax.rsqrt(jnp.mean(resid * resid, axis=-1, keepdims=True) + 1e-06)
    mid = (resid * scale * gain[...][None, :]).astype(BF16)
    gated = jnp.sum(mid.astype(F32) * blend_vec[...][None, :].astype(F32), axis=-1, keepdims=True)
    table = jnp.where(lanes == count, sigmoid(gated), table)
    high = table.astype(BF16)
    gbuf[0, e, :, :half] = mid[:, :half]
    gbuf[1, e, :, :half] = mid[:, half:]
    gbuf[0, e, :, half:] = high
    gbuf[1, e, :, half:] = (table - high.astype(F32)).astype(BF16)

    def block(o, send, device):
        return remote(gbuf.at[t, o], gbuf.at[t, o], send, agr.at[o], device)

    def forward(o):
        return remote(gbuf.at[t, o], gbuf.at[t, o], fs.at[o], fr.at[o], (e, other))

    for dz in range(1, depth):
        block(e, zs.at[dz], (at_z(dz) * plane + p, t)).start()
    for dp in range(1, plane):
        block(e, ps.at[0, dp], (z * plane + at_p(dp), t)).start()
    for dz in range(1, depth):
        o = at_z(dz) * plane + p
        block(o, zs.at[dz], (e, other)).wait_recv()
        for dp in range(1, plane):
            block(o, ps.at[dz, dp], (z * plane + at_p(dp), t)).start()
        forward(o).start()
    for dz in range(depth):
        for dp in range(1, plane):
            o = at_z(dz) * plane + at_p(dp)
            block(o, zs.at[0], (e, other)).wait_recv()
            forward(o).start()
    for dz in range(depth):
        for dp in range(plane):
            if dz or dp:
                o = at_z(dz) * plane + at_p(dp)
                remote(
                    gbuf.at[other, o], gbuf.at[other, o], fs.at[o], fr.at[o], (e, other)
                ).wait_recv()
    for copy in weights:
        copy.wait()

    group = min(count, 16)
    size = group * seqs

    def hidden(c, carry):
        where = pl.ds(c * group, group)
        x0 = gbuf[0, where, :, :half].reshape(size, half)
        x1 = gbuf[1, where, :, :half].reshape(size, half)
        tab = gbuf[0, where, :, half:].astype(F32) + gbuf[1, where, :, half:].astype(F32)
        tab = tab.reshape(size, tail)
        lane = lax.broadcasted_iota(jnp.int32, (size, tail), 1)

        def pick(slot):
            return jnp.sum(jnp.where(lane == slot, tab, 0.0), axis=1, keepdims=True)

        def branch(gate, up, factor):
            g = dot_t(x0, gate[:, :half]) + dot_t(x1, gate[:, half:])
            u = dot_t(x0, up[:, :half]) + dot_t(x1, up[:, half:])
            return (g * sigmoid(g) * u * factor).astype(BF16).reshape(group, seqs, -1)

        hid_e[where] = branch(eg_v, eu_v, pick(e))
        hid_d[where] = branch(dg_v, du_v, pick(count))
        return carry

    lax.fori_loop(0, count // group, hidden, 0)

    def to_partner(c):
        return remote(ds2.at[c], dr2.at[c], d2s.at[c], d2r.at[c], (e, other))

    mine_at = pl.ds(pl.multiple_of(t * half, 128), half)
    theirs_at = pl.ds(pl.multiple_of(other * half, 128), half)

    def down(i, carry):
        c = at_z(i + 1)
        he = hid_e[pl.ds(c * plane, plane)].reshape(plane * seqs, -1)
        hd = hid_d[pl.ds(c * plane, plane)].reshape(plane * seqs, -1)
        theirs = dot(he, ed_v[:, theirs_at]) + dot(hd, dn_v[:, theirs_at])
        ds2[c] = theirs.astype(BF16).reshape(plane, seqs, half)
        to_partner(c).start()
        mine = dot(he, ed_v[:, mine_at]) + dot(hd, dn_v[:, mine_at])
        own[c] = mine.reshape(plane, seqs, half)
        return carry

    lax.fori_loop(0, depth, down, 0)

    def in_plane(c, dp):
        q = at_p(dp)
        return remote(r1s.at[c, q], r1r.at[c, p], s1.at[c, q], r1.at[c, p], (z * plane + q, t))

    def spread(i, carry):
        c = at_z(i + 1)
        to_partner(c).wait_recv()
        total = own[c] + dr2[c].astype(F32)
        own[c] = total
        r1s[c] = total.astype(BF16)
        for dp in range(1, plane):
            in_plane(c, dp).start()
        return carry

    lax.fori_loop(0, depth, spread, 0)

    def along_z(c):
        return remote(r2s.at[c], r2r.at[z], s2.at[c], r2.at[z], (c * plane + p, t))

    acc = None
    for i in range(depth):
        c = at_z(i + 1)
        acc = own[c, p]
        for dp in range(1, plane):
            q = at_p(dp)
            remote(r1s.at[c, q], r1r.at[c, q], s1.at[c, q], r1.at[c, q], (e, other)).wait_recv()
            acc = acc + r1r[c, q].astype(F32)
        if i < depth - 1:
            r2s[c] = acc.astype(BF16)
            along_z(c).start()
    for i in range(depth - 1):
        c = at_z(i + 1)
        remote(r2s.at[c], r2r.at[c], s2.at[c], r2.at[c], (e, other)).wait_recv()
        acc = acc + r2r[c].astype(F32)
    out[...] = (res[t] + acc).astype(BF16)

    for dz in range(1, depth):
        block(e, zs.at[dz], (at_z(dz) * plane + p, t)).wait_send()
        along_z(at_z(dz)).wait_send()
    for dz in range(depth):
        to_partner(at_z(dz)).wait_send()
        for dp in range(plane):
            o = at_z(dz) * plane + at_p(dp)
            if dp:
                block(at_z(dz) * plane + p, ps.at[dz, dp], (z * plane + at_p(dp), t)).wait_send()
                in_plane(at_z(dz), dp).wait_send()
            if dz or dp:
                forward(o).wait_send()


def shards(
    tokens, prior_state, first_gain, query_weight, key_weight, value_weight,
    decay_down, decay_up, decay_base, rate_down, rate_up, rate_base, head_gain,
    out_weight, mid_gain, route_ids, route_weights, expert_gate, expert_up, expert_down,
    dense_gate, dense_up, dense_down, blend_vector,
):
    count = lax.axis_size("ep")
    assert lax.axis_size("tp") == 2
    seqs, width = tokens.shape
    half = width // 2
    heads, size = prior_state.shape[1], prior_state.shape[2]
    inner = heads * size
    dma = pltpu.SemaphoreType.DMA
    part, new_state = pl.pallas_call(
        front_kernel,
        name="front",
        out_shape=(
            jax.ShapeDtypeStruct((seqs, width), BF16),
            jax.ShapeDtypeStruct(prior_state.shape, F32),
        ),
        in_specs=[VMEM, ANY, VMEM, ANY, ANY, ANY] + [VMEM] * 7 + [ANY],
        out_specs=(VMEM, ANY),
        scratch_shapes=[
            pltpu.VMEM((width, inner), BF16),
            pltpu.VMEM((width, inner), BF16),
            pltpu.VMEM((width, inner), BF16),
            pltpu.VMEM((inner, width), BF16),
            pltpu.VMEM(prior_state.shape, F32),
            pltpu.VMEM(prior_state.shape, F32),
            pltpu.VMEM((6, heads, seqs, size), F32),
            pltpu.VMEM((heads, seqs, size), F32),
            dma((4,)),
            dma((seqs,)),
            dma((seqs,)),
        ],
        compiler_params=pltpu.CompilerParams(vmem_limit_bytes=67043328),
    )(
        tokens, prior_state, first_gain, query_weight, key_weight, value_weight,
        decay_down.T, decay_up, decay_base, rate_down.T, rate_up, rate_base, head_gain, out_weight,
    )

    plane = 1
    while (plane * 2) ** 2 <= count and count % (plane * 2) == 0:
        plane *= 2
    depth = count // plane
    fe = expert_gate.shape[2]
    fd = dense_gate.shape[1]
    tail = -(-(count + 1) // 128) * 128
    mixed = pl.pallas_call(
        functools.partial(back_kernel, count, plane),
        name="back",
        out_shape=jax.ShapeDtypeStruct((seqs, half), BF16),
        in_specs=[VMEM] * 6 + [ANY] * 6,
        out_specs=VMEM,
        scratch_shapes=[
            pltpu.VMEM((fe, width), BF16),
            pltpu.VMEM((fe, width), BF16),
            pltpu.VMEM((fe, width), BF16),
            pltpu.VMEM((fd, width), BF16),
            pltpu.VMEM((fd, width), BF16),
            pltpu.VMEM((fd, width), BF16),
            pltpu.VMEM((seqs, width), BF16),
            pltpu.VMEM((2, count, seqs, half + tail), BF16),
            pltpu.VMEM((2, seqs, half), F32),
            pltpu.VMEM((count, seqs, fe), BF16),
            pltpu.VMEM((count, seqs, fd), BF16),
            pltpu.VMEM((depth, plane, seqs, half), F32),
            pltpu.VMEM((depth, plane, seqs, half), BF16),
            pltpu.VMEM((depth, plane, seqs, half), BF16),
            pltpu.VMEM((depth, plane, seqs, half), BF16),
            pltpu.VMEM((depth, plane, seqs, half), BF16),
            pltpu.VMEM((depth, seqs, half), BF16),
            pltpu.VMEM((depth, seqs, half), BF16),
            dma((6,)),
            dma,
            dma,
            dma((count,)),
            dma((depth,)),
            dma((depth, plane)),
            dma((count,)),
            dma((count,)),
            dma((depth,)),
            dma((depth,)),
            dma((depth, plane)),
            dma((depth, plane)),
            dma((depth,)),
            dma((depth,)),
        ],
        compiler_params=pltpu.CompilerParams(
            collective_id=0, has_side_effects=True, vmem_limit_bytes=67043328
        ),
    )(
        tokens, part, mid_gain, route_ids.T, route_weights.T, blend_vector,
        jnp.swapaxes(expert_gate, 1, 2), jnp.swapaxes(expert_up, 1, 2), expert_down,
        dense_gate.T, dense_up.T, dense_down,
    )
    return (mixed, new_state)


def solution(mesh):
    in_specs = (
        P("ep", None),
        P("ep", "tp", None, None),
        P(),
        P(None, "tp"),
        P(None, "tp"),
        P(None, "tp"),
        P(),
        P(None, "tp"),
        P("tp"),
        P(),
        P(None, "tp"),
        P("tp"),
        P("tp"),
        P("tp", None),
        P(),
        P("ep", None),
        P("ep", None),
        P("ep", None, "tp"),
        P("ep", None, "tp"),
        P("ep", "tp", None),
        P(None, ("ep", "tp")),
        P(None, ("ep", "tp")),
        P(("ep", "tp"), None),
        P(),
    )
    out_specs = (P("ep", "tp"), P("ep", "tp", None, None))
    return jax.shard_map(shards, mesh=mesh, in_specs=in_specs, out_specs=out_specs, check_vma=False)
```

```python
import functools

import jax
import jax.numpy as jnp
from jax import lax
from jax.experimental import pallas as pl
from jax.experimental.pallas import tpu as pltpu
from jax.sharding import PartitionSpec as P

MESH = pl.DeviceIdType.MESH
F32 = jnp.float32
BF16 = jnp.bfloat16
ANY = pl.BlockSpec(memory_space=pl.ANY)
VMEM = pl.BlockSpec(memory_space=pltpu.VMEM)


def dot(a, b):
    return jnp.dot(a, b, preferred_element_type=F32)


def dot_t(a, b):
    return lax.dot_general(a, b, (((1,), (1,)), ((), ())), preferred_element_type=F32)


def sigmoid(x):
    return 1.0 / (1.0 + jnp.exp(-x))


def front_kernel(
    tok, state, gain, wq, wk, wv, dd, du, db, rd, ru, rb, hg, ow,
    part, new_state,
    q_v, k_v, v_v, ow_v, st, sto, vec, reads, wsem, isem, osem,
):
    rows, heads, size = st.shape[0], st.shape[1], st.shape[2]
    weights = [
        pltpu.make_async_copy(src, dst, wsem.at[i])
        for i, (src, dst) in enumerate(((wk, k_v), (wq, q_v), (wv, v_v), (ow, ow_v)))
    ]
    for copy in weights[:3]:
        copy.start()

    def state_in(r):
        return pltpu.make_async_copy(state.at[r], st.at[r], isem.at[r])

    def state_out(r):
        return pltpu.make_async_copy(sto.at[r], new_state.at[r], osem.at[r])

    for r in range(rows):
        state_in(r).start()
    weights[3].start()

    x = tok[...].astype(F32)
    scale = lax.rsqrt(jnp.mean(x * x, axis=-1, keepdims=True) + 1e-06)
    normed = (x * scale * gain[...][None, :]).astype(BF16)
    low = jnp.tanh(dot_t(normed, dd[...])).astype(BF16)
    decay = jnp.exp(-0.6065306597126334 * sigmoid(db[...][None, :] + dot(low, du[...])))
    rlow = dot_t(normed, rd[...]).astype(BF16)
    rate = sigmoid(rb[...][None, :] + dot(rlow, ru[...]))
    weights[0].wait()
    key = dot(normed, k_v[...]).astype(BF16).astype(F32)
    weights[1].wait()
    rec = dot(normed, q_v[...]).astype(BF16).astype(F32)
    weights[2].wait()
    val = dot(normed, v_v[...]).astype(BF16).astype(F32)
    for h in range(heads):
        at = slice(h * size, (h + 1) * size)
        kh = key[:, at]
        unit = kh * lax.rsqrt(jnp.sum(kh * kh, axis=-1, keepdims=True) + 1e-06)
        vec[0, h] = unit
        vec[1, h] = decay[:, at]
        vec[2, h] = unit * rate[:, at]
        vec[3, h] = kh
        vec[4, h] = rec[:, at]
        vec[5, h] = val[:, at]

    eye = lax.broadcasted_iota(jnp.int32, (size, size), 0) == lax.broadcasted_iota(
        jnp.int32, (size, size), 1
    )

    unity = jnp.where(eye, 1.0, 0.0).astype(BF16)

    batch = 2

    def step(i, carry):
        for b in range(batch):
            state_in(i * batch + b).wait()
        for b in range(batch):
            r = i * batch + b
            for h in range(heads):
                unit, dec, ul, kh, qh, vh = [vec[j, h, pl.ds(r, 1), :] for j in range(6)]
                s = st[r, h]
                removed = jnp.sum(s * unit, axis=-1, keepdims=True)
                vcol = dot_t(unity, jnp.broadcast_to(vh, (size, size)).astype(BF16))
                new = s * dec - removed * ul + vcol * kh
                sto[r, h] = new
                read = jnp.sum(new * qh, axis=-1, keepdims=True)
                reads[h, pl.ds(r, 1), :] = jnp.sum(jnp.where(eye, read, 0.0), axis=0, keepdims=True)
        for b in range(batch):
            state_out(i * batch + b).start()
        return carry

    lax.fori_loop(0, rows // batch, step, 0)
    weights[3].wait()
    total = None
    for h in range(heads):
        at = slice(h * size, (h + 1) * size)
        read = reads[h]
        read = read - jnp.mean(read, axis=-1, keepdims=True)
        spread = jnp.mean(read * read, axis=-1, keepdims=True)
        mixed = (read * lax.rsqrt(spread + 0.00064) * hg[...][None, :][:, at]).astype(BF16)
        term = dot(mixed, ow_v[h * size : (h + 1) * size, :])
        total = term if total is None else total + term
    part[...] = total.astype(BF16)

    def drain(r, carry):
        state_out(r).wait()
        return carry

    lax.fori_loop(0, rows, drain, 0)


def back_kernel(
    count, plane,
    tok, part, gain, ids, scores, blend_vec, eg, eu, ed, dg, du, dn,
    out,
    eg_v, eu_v, ed_v, dg_v, du_v, dn_v, prx, gbuf, res, hid_e, hid_d, own, ds2, dr2, r1s, r1r, r2s, r2r,
    wsem, xs, xr, agr, zs, ps, fs, fr, d2s, d2r, s1, r1, s2, r2,
):
    e = lax.axis_index("ep")
    t = lax.axis_index("tp")
    other = 1 - t
    depth = count // plane
    z, p = e // plane, e % plane
    seqs, width = tok.shape
    half = width // 2
    tail = gbuf.shape[3] - half
    top = ids.shape[0]

    barrier = pltpu.get_barrier_semaphore()

    def greet(device):
        pl.semaphore_signal(barrier, inc=1, device_id=device, device_id_type=MESH)

    def at_z(dz):
        return (z + dz) % depth

    def at_p(dp):
        return (p + dp) % plane

    def near(j):
        low = j + (j - z + depth) // depth
        flipped = depth - 1 - z
        high = depth - 1 - (j + (j - flipped + depth) // depth)
        return low + (2 * z) // depth * (high - low)

    def far(i):
        last = (i + 1) // depth
        return (1 - last) * near((1 - last) * (depth - 2 - i)) + last * z

    greet((e, other))
    for dz in range(1, depth):
        greet((at_z(dz) * plane + p, t))
    for dp in range(1, plane):
        greet((z * plane + at_p(dp), t))

    weights = [
        pltpu.make_async_copy(src, dst, wsem.at[i])
        for i, (src, dst) in enumerate(
            ((eg.at[0], eg_v), (eu.at[0], eu_v), (dg, dg_v), (du, du_v), (ed.at[0], ed_v), (dn, dn_v))
        )
    ]
    for copy in weights:
        copy.start()

    def remote(src, dst, send, recv, device):
        return pltpu.make_async_remote_copy(
            src_ref=src, dst_ref=dst, send_sem=send, recv_sem=recv,
            device_id=device, device_id_type=MESH,
        )

    lanes = lax.broadcasted_iota(jnp.int32, (seqs, tail), 1)
    score = scores[...]
    share = score / jnp.sum(score, axis=0, keepdims=True) * 2.5
    id_all = ids[...].astype(F32)
    eye = lax.broadcasted_iota(jnp.int32, (seqs, seqs), 0) == lax.broadcasted_iota(
        jnp.int32, (seqs, seqs), 1
    )

    def column(row):
        return jnp.sum(jnp.where(eye, row, 0.0), axis=1, keepdims=True)

    table = jnp.zeros((seqs, tail), F32)
    for k in range(top):
        named = lanes.astype(F32) == column(id_all[k : k + 1, :])
        table = table + jnp.where(named, column(share[k : k + 1, :]), 0.0)

    pl.semaphore_wait(barrier, 1 + (depth - 1) + (plane - 1))
    swap = remote(part, prx, xs, xr, (e, other))
    swap.start()
    token_f = tok[...].astype(F32)
    swap.wait()
    resid = (token_f + (part[...].astype(F32) + prx[...].astype(F32))).astype(BF16).astype(F32)
    res[0] = resid[:, :half]
    res[1] = resid[:, half:]
    scale = lax.rsqrt(jnp.mean(resid * resid, axis=-1, keepdims=True) + 1e-06)
    mid = (resid * scale * gain[...][None, :]).astype(BF16)
    gated = jnp.sum(mid.astype(F32) * blend_vec[...][None, :].astype(F32), axis=-1, keepdims=True)
    table = jnp.where(lanes == count, sigmoid(gated), table)
    high = table.astype(BF16)
    gbuf[0, e, :, :half] = mid[:, :half]
    gbuf[1, e, :, :half] = mid[:, half:]
    gbuf[0, e, :, half:] = high
    gbuf[1, e, :, half:] = (table - high.astype(F32)).astype(BF16)

    def block(o, send, device):
        return remote(gbuf.at[t, o], gbuf.at[t, o], send, agr.at[o], device)

    def forward(o):
        return remote(gbuf.at[t, o], gbuf.at[t, o], fs.at[o], fr.at[o], (e, other))

    for j in range(depth - 2, -1, -1):
        block(e, zs.at[j + 1], (near(j) * plane + p, t)).start()
    for dp in range(1, plane):
        block(e, ps.at[0, dp], (z * plane + at_p(dp), t)).start()
    for dz in range(1, depth):
        o = near(dz - 1) * plane + p
        block(o, zs.at[dz], (e, other)).wait_recv()
        for dp in range(1, plane):
            block(o, ps.at[dz, dp], (z * plane + at_p(dp), t)).start()
        forward(o).start()
    for dz in range(depth):
        for dp in range(1, plane):
            o = (near(dz - 1) if dz else z) * plane + at_p(dp)
            block(o, zs.at[0], (e, other)).wait_recv()
            forward(o).start()
    for dz in range(depth):
        for dp in range(plane):
            if dz or dp:
                o = at_z(dz) * plane + at_p(dp)
                remote(
                    gbuf.at[other, o], gbuf.at[other, o], fs.at[o], fr.at[o], (e, other)
                ).wait_recv()
    for copy in weights:
        copy.wait()

    group = min(count, 16)
    size = group * seqs

    def hidden(c, carry):
        where = pl.ds(c * group, group)
        x0 = gbuf[0, where, :, :half].reshape(size, half)
        x1 = gbuf[1, where, :, :half].reshape(size, half)
        tab = gbuf[0, where, :, half:].astype(F32) + gbuf[1, where, :, half:].astype(F32)
        tab = tab.reshape(size, tail)
        lane = lax.broadcasted_iota(jnp.int32, (size, tail), 1)

        def pick(slot):
            return jnp.sum(jnp.where(lane == slot, tab, 0.0), axis=1, keepdims=True)

        def branch(gate, up, factor):
            g = dot_t(x0, gate[:, :half]) + dot_t(x1, gate[:, half:])
            u = dot_t(x0, up[:, :half]) + dot_t(x1, up[:, half:])
            return (g * sigmoid(g) * u * factor).astype(BF16).reshape(group, seqs, -1)

        hid_e[where] = branch(eg_v, eu_v, pick(e))
        hid_d[where] = branch(dg_v, du_v, pick(count))
        return carry

    lax.fori_loop(0, count // group, hidden, 0)

    def to_partner(c):
        return remote(ds2.at[c], dr2.at[c], d2s.at[c], d2r.at[c], (e, other))

    mine_at = pl.ds(pl.multiple_of(t * half, 128), half)
    theirs_at = pl.ds(pl.multiple_of(other * half, 128), half)

    def down(i, carry):
        c = far(i)
        he = hid_e[pl.ds(c * plane, plane)].reshape(plane * seqs, -1)
        hd = hid_d[pl.ds(c * plane, plane)].reshape(plane * seqs, -1)
        theirs = dot(he, ed_v[:, theirs_at]) + dot(hd, dn_v[:, theirs_at])
        ds2[c] = theirs.astype(BF16).reshape(plane, seqs, half)
        to_partner(c).start()
        mine = dot(he, ed_v[:, mine_at]) + dot(hd, dn_v[:, mine_at])
        own[c] = mine.reshape(plane, seqs, half)
        return carry

    lax.fori_loop(0, depth, down, 0)

    def in_plane(c, dp):
        q = at_p(dp)
        return remote(r1s.at[c, q], r1r.at[c, p], s1.at[c, q], r1.at[c, p], (z * plane + q, t))

    def spread(i, carry):
        c = far(i)
        to_partner(c).wait_recv()
        total = own[c] + dr2[c].astype(F32)
        own[c] = total
        r1s[c] = total.astype(BF16)
        for dp in range(1, plane):
            in_plane(c, dp).start()
        return carry

    lax.fori_loop(0, depth, spread, 0)

    def along_z(c):
        return remote(r2s.at[c], r2r.at[z], s2.at[c], r2.at[z], (c * plane + p, t))

    acc = None
    for i in range(depth):
        c = far(i)
        acc = own[c, p]
        for dp in range(1, plane):
            q = at_p(dp)
            remote(r1s.at[c, q], r1r.at[c, q], s1.at[c, q], r1.at[c, q], (e, other)).wait_recv()
            acc = acc + r1r[c, q].astype(F32)
        if i < depth - 1:
            r2s[c] = acc.astype(BF16)
            along_z(c).start()
    for i in range(depth - 1):
        c = near(i)
        remote(r2s.at[c], r2r.at[c], s2.at[c], r2.at[c], (e, other)).wait_recv()
        acc = acc + r2r[c].astype(F32)
    out[...] = (res[t] + acc).astype(BF16)

    for dz in range(1, depth):
        block(e, zs.at[dz], (at_z(dz) * plane + p, t)).wait_send()
        along_z(at_z(dz)).wait_send()
    for dz in range(depth):
        to_partner(at_z(dz)).wait_send()
        for dp in range(plane):
            o = at_z(dz) * plane + at_p(dp)
            if dp:
                block(at_z(dz) * plane + p, ps.at[dz, dp], (z * plane + at_p(dp), t)).wait_send()
                in_plane(at_z(dz), dp).wait_send()
            if dz or dp:
                forward(o).wait_send()


def shards(
    tokens, prior_state, first_gain, query_weight, key_weight, value_weight,
    decay_down, decay_up, decay_base, rate_down, rate_up, rate_base, head_gain,
    out_weight, mid_gain, route_ids, route_weights, expert_gate, expert_up, expert_down,
    dense_gate, dense_up, dense_down, blend_vector,
):
    count = lax.axis_size("ep")
    assert lax.axis_size("tp") == 2
    seqs, width = tokens.shape
    half = width // 2
    heads, size = prior_state.shape[1], prior_state.shape[2]
    inner = heads * size
    dma = pltpu.SemaphoreType.DMA
    part, new_state = pl.pallas_call(
        front_kernel,
        name="front",
        out_shape=(
            jax.ShapeDtypeStruct((seqs, width), BF16),
            jax.ShapeDtypeStruct(prior_state.shape, F32),
        ),
        in_specs=[VMEM, ANY, VMEM, ANY, ANY, ANY] + [VMEM] * 7 + [ANY],
        out_specs=(VMEM, ANY),
        scratch_shapes=[
            pltpu.VMEM((width, inner), BF16),
            pltpu.VMEM((width, inner), BF16),
            pltpu.VMEM((width, inner), BF16),
            pltpu.VMEM((inner, width), BF16),
            pltpu.VMEM(prior_state.shape, F32),
            pltpu.VMEM(prior_state.shape, F32),
            pltpu.VMEM((6, heads, seqs, size), F32),
            pltpu.VMEM((heads, seqs, size), F32),
            dma((4,)),
            dma((seqs,)),
            dma((seqs,)),
        ],
        compiler_params=pltpu.CompilerParams(vmem_limit_bytes=67043328),
    )(
        tokens, prior_state, first_gain, query_weight, key_weight, value_weight,
        decay_down.T, decay_up, decay_base, rate_down.T, rate_up, rate_base, head_gain, out_weight,
    )

    plane = 1
    while (plane * 2) ** 2 <= count and count % (plane * 2) == 0:
        plane *= 2
    depth = count // plane
    fe = expert_gate.shape[2]
    fd = dense_gate.shape[1]
    tail = -(-(count + 1) // 128) * 128
    mixed = pl.pallas_call(
        functools.partial(back_kernel, count, plane),
        name="back",
        out_shape=jax.ShapeDtypeStruct((seqs, half), BF16),
        in_specs=[VMEM] * 6 + [ANY] * 6,
        out_specs=VMEM,
        scratch_shapes=[
            pltpu.VMEM((fe, width), BF16),
            pltpu.VMEM((fe, width), BF16),
            pltpu.VMEM((fe, width), BF16),
            pltpu.VMEM((fd, width), BF16),
            pltpu.VMEM((fd, width), BF16),
            pltpu.VMEM((fd, width), BF16),
            pltpu.VMEM((seqs, width), BF16),
            pltpu.VMEM((2, count, seqs, half + tail), BF16),
            pltpu.VMEM((2, seqs, half), F32),
            pltpu.VMEM((count, seqs, fe), BF16),
            pltpu.VMEM((count, seqs, fd), BF16),
            pltpu.VMEM((depth, plane, seqs, half), F32),
            pltpu.VMEM((depth, plane, seqs, half), BF16),
            pltpu.VMEM((depth, plane, seqs, half), BF16),
            pltpu.VMEM((depth, plane, seqs, half), BF16),
            pltpu.VMEM((depth, plane, seqs, half), BF16),
            pltpu.VMEM((depth, seqs, half), BF16),
            pltpu.VMEM((depth, seqs, half), BF16),
            dma((6,)),
            dma,
            dma,
            dma((count,)),
            dma((depth,)),
            dma((depth, plane)),
            dma((count,)),
            dma((count,)),
            dma((depth,)),
            dma((depth,)),
            dma((depth, plane)),
            dma((depth, plane)),
            dma((depth,)),
            dma((depth,)),
        ],
        compiler_params=pltpu.CompilerParams(
            collective_id=0, has_side_effects=True, vmem_limit_bytes=67043328
        ),
    )(
        tokens, part, mid_gain, route_ids.T, route_weights.T, blend_vector,
        jnp.swapaxes(expert_gate, 1, 2), jnp.swapaxes(expert_up, 1, 2), expert_down,
        dense_gate.T, dense_up.T, dense_down,
    )
    return (mixed, new_state)


def solution(mesh):
    in_specs = (
        P("ep", None),
        P("ep", "tp", None, None),
        P(),
        P(None, "tp"),
        P(None, "tp"),
        P(None, "tp"),
        P(),
        P(None, "tp"),
        P("tp"),
        P(),
        P(None, "tp"),
        P("tp"),
        P("tp"),
        P("tp", None),
        P(),
        P("ep", None),
        P("ep", None),
        P("ep", None, "tp"),
        P("ep", None, "tp"),
        P("ep", "tp", None),
        P(None, ("ep", "tp")),
        P(None, ("ep", "tp")),
        P(("ep", "tp"), None),
        P(),
    )
    out_specs = (P("ep", "tp"), P("ep", "tp", None, None))
    return jax.shard_map(shards, mesh=mesh, in_specs=in_specs, out_specs=out_specs, check_vma=False)
```
